128 devices in a mesh: fs: 32 (over z, y, core), tp: 4 (over x).
Axes of the slice: x: 4, y: 4, z: 4, core: 2. Of those that a mesh axis runs over, the one named last changes fastest.
Arguments:
- tokens: bfloat16 [32768, 2048], P('fs'), may hold values from -6 to 6
- norm_gain: float32 [2048], P('fs'), may hold values from 0.1 to 1.9
- gate_train: float32 [32, 2048, 768], P(None, 'fs', 'tp'), may hold values from -0.125 to 0.125
- up_train: float32 [32, 2048, 768], P(None, 'fs', 'tp'), may hold values from -0.125 to 0.125
- down_train: float32 [32, 768, 2048], P(None, 'fs', 'tp'), may hold values from -0.21875 to 0.21875
- expert_ids: int32 [32768, 2], P('fs'), may hold values from 0 to 31, all different within a row; in each aligned block of 1024 rows (0 to 1023, 1024 to 2047, ...) at most 128 rows name the same one
- route_weights: float32 [32768, 2], P('fs'), may hold values from 0.1 to 1
Outputs:
- gate_serve: bfloat16 [32, 2048, 768], P('fs', None, 'tp')
- up_serve: bfloat16 [32, 2048, 768], P('fs', None, 'tp')
- down_serve: bfloat16 [32, 768, 2048], P('fs', 'tp')
- mixed: bfloat16 [32768, 2048], P('fs', 'tp')
The draws below stay inside these ranges and needn't reach their ends.
Inputs may be any that keep to these rules, and one draw needn't show every extreme that they name: `expert_ids`: each row names 2 different experts. Within each aligned block of 1024 rows no expert is named more than 128 times, and in every block some expert is named exactly 128 times; every expert is named somewhere.
All inputs are finite; a program needn't handle non-finite values.
Results may differ from the reference program's by a relative error of at most 0.011.
Values may be sent and summed in bfloat16 or wider, within the bound.
A program may use at most 128 MiB of HBM per device.

```python
import math
import jax
import jax.numpy as jnp
import numpy as np
from jax import lax

D = 2048
FF = 768
TOP = 2
TOK_DEV = 1024
EXPERTS = 32
CAP = 128
TOKENS = 32768
N_FS = 32
N_TP = 4


def shard_levels(key, shape, shards, least, top_value):
    loudness = 1.0
    for axis_at, parts in shards:
        draws = jax.random.uniform(jax.random.fold_in(jax.random.fold_in(key, 6), axis_at), (parts,), jnp.float32, least / len(shards), top_value / len(shards))
        loudness = loudness * jnp.repeat(jnp.exp(draws), shape[axis_at] // parts).reshape((-1,) + (1,) * (len(shape) - 1 - axis_at))
    return loudness


def shared_out(own_key, own, number, rows, number_of, top, limit, lean):
    ranking = jax.random.permutation(own_key, number_of)
    heavy_load, ordinary = portions_of(number_of, rows * top, limit, lean, True), portions_of(number_of, rows * top, limit, lean, False)
    places = jnp.arange(number_of)

    def named(sizes, offset_by):
        used = int((sizes > 0).sum())
        fixed = max(1, used // 4)
        moved = fixed + (places - fixed + offset_by * (used - fixed)) % max(1, number_of - fixed)
        return jnp.zeros((number_of,), jnp.int32).at[ranking[jnp.where(places < fixed, places, moved)]].set(jnp.asarray(sizes, jnp.int32))

    sizes = jnp.where(number % 4 == 0, named(heavy_load, number // 4), named(ordinary, number - number // 4 - 1))
    mixed = jax.random.permutation(jax.random.fold_in(own, 3), number_of)
    source_of, sink = mixed[0:number_of // 2 * 2:2], mixed[1:number_of // 2 * 2:2]
    slack = jnp.minimum(sizes[source_of] - 1, limit - sizes[sink]) // 2
    slack = jnp.where((source_of == ranking[0]) | (sink == ranking[0]) | (sizes[sink] == 0), 0, jnp.maximum(slack, 0))
    moved = jax.random.randint(jax.random.fold_in(own, 4), (number_of // 2,), 0, 1 << 20) % (slack + 1)
    sizes = sizes.at[source_of].add(-moved).at[sink].add(moved)
    items = jnp.searchsorted(jnp.cumsum(sizes), jnp.arange(rows * top), side="right").astype(jnp.int32)
    table = items.reshape(top, rows).T
    table = table[jax.random.permutation(jax.random.fold_in(own, 1), rows)]
    offset_by = jax.random.randint(jax.random.fold_in(own, 2), (rows, 1), 0, top)
    return jnp.take_along_axis(table, (jnp.arange(top)[None, :] + offset_by) % top, axis=1)


def portions_of(number_of, total, limit, slope, full):
    portions = [(1 << 20) // math.isqrt(standing ** slope) + 1 for standing in range(1, number_of + 1)]
    largest = limit if full else min(limit, max(-(-total // number_of), total * portions[0] // sum(portions)))
    least = 1 if total - largest >= number_of - 1 else 0
    counts, rest = [largest] + [least] * (number_of - 1), total - largest - least * (number_of - 1)
    while rest > 0:
        movable = [i for i in range(1, number_of) if counts[i] < largest] or [i for i in range(1, number_of) if counts[i] < limit]
        mass, budget = sum([portions[i] for i in movable]), rest
        for i in movable:
            addition = min(limit - counts[i], max(1, budget * portions[i] // mass), rest)
            counts[i] = counts[i] + addition
            rest = rest - addition
    return np.array(counts)


def bell_draw(rng, dims, spread, reach, pieces=(), held_as=jnp.bfloat16):
    entries = jax.random.normal(rng, dims, jnp.float32) * spread
    if len(pieces) > 0:
        entries = shard_levels(rng, dims, pieces, -0.22, 0.18) * entries
    return jnp.clip(entries, min=-reach, max=reach).astype(held_as)


def setup_inputs(seed: int = 0) -> dict:
    keys = jax.random.split(jax.random.key(seed), 8)
    tokens = bell_draw(keys[0], (TOKENS, D), 1.0, 6.0, ((0, 32),))
    norm_gain = jnp.clip(1.0 + 0.18 * jax.random.normal(keys[1], (D,), jnp.float32), 0.1, 1.9)
    gate_train = bell_draw(keys[2], (EXPERTS, D, FF), D ** -0.5, 0.125, ((1, 32), (2, 4)), jnp.float32)
    up_train = bell_draw(keys[3], (EXPERTS, D, FF), D ** -0.5, 0.125, ((1, 32), (2, 4)), jnp.float32)
    down_train = bell_draw(keys[4], (EXPERTS, FF, D), FF ** -0.5, 0.21875, ((1, 32), (2, 4)), jnp.float32)
    expert_ids_keys = jax.random.split(jax.random.fold_in(keys[5], 1), TOKENS // TOK_DEV)
    expert_ids_turns = jax.random.permutation(jax.random.fold_in(keys[5], 3), TOKENS // TOK_DEV)
    expert_ids = jax.vmap(lambda own, number: shared_out(jax.random.fold_in(keys[5], 2), own, number, TOK_DEV, EXPERTS, TOP, CAP, 2))(expert_ids_keys, expert_ids_turns).reshape((TOKENS, TOP))
    route_weights = jnp.clip(jnp.exp(math.log(1.0) - 2.3025851 * jax.random.uniform(keys[6], (TOKENS, TOP), jnp.float32) ** shard_levels(keys[6], (TOKENS, TOP), ((0, 32),), -0.2, 0.2)), 0.1, 1.0)
    return dict(tokens=tokens, norm_gain=norm_gain, gate_train=gate_train, up_train=up_train, down_train=down_train, expert_ids=expert_ids, route_weights=route_weights)


epsilon = 1e-06

def reference(tokens, norm_gain, gate_train, up_train, down_train, expert_ids, route_weights):
    gate_serve = (norm_gain[None, :, None] * gate_train).astype(jnp.bfloat16)
    up_serve = (norm_gain[None, :, None] * up_train).astype(jnp.bfloat16)
    down_serve = down_train.astype(jnp.bfloat16)
    tok_float = tokens.astype(jnp.float32)
    normed = (tok_float * lax.rsqrt(lax.optimization_barrier(jnp.mean(tok_float * tok_float, axis=-1, keepdims=True)) + epsilon)).astype(jnp.bfloat16)
    flat_ids = expert_ids.reshape(N_FS, TOK_DEV * TOP)
    onehot = (flat_ids[:, :, None] == jnp.arange(EXPERTS, dtype=jnp.int32)[None, None, :]).astype(jnp.int32)
    slot_rank = lax.optimization_barrier(jnp.sum((jnp.cumsum(onehot, axis=1) - onehot) * onehot, axis=-1))
    row_index = (jnp.arange(N_FS, dtype=jnp.int32)[:, None] * CAP + slot_rank).astype(jnp.int32)
    tok_index = (jnp.arange(N_FS, dtype=jnp.int32)[:, None] * TOK_DEV + jnp.arange(TOK_DEV * TOP, dtype=jnp.int32)[None, :] // TOP).astype(jnp.int32)
    buffer = jnp.zeros((EXPERTS, N_FS * CAP, D), jnp.bfloat16)
    buffer = buffer.at[flat_ids.reshape(-1), row_index.reshape(-1)].set(normed[tok_index.reshape(-1)])
    block_width = FF // N_TP

    def expert_apply(inputs):
        routed, weight_gate, weight_up, weight_down = inputs
        gate_act = jnp.dot(routed, weight_gate, preferred_element_type=jnp.float32)
        up_act = jnp.dot(routed, weight_up, preferred_element_type=jnp.float32)
        hidden = (jax.nn.silu(gate_act) * up_act).astype(jnp.bfloat16)
        running = jnp.zeros((routed.shape[0], D), jnp.float32)
        for index_tp in range(N_TP):
            partial_value = jnp.dot(hidden[:, index_tp * block_width:(index_tp + 1) * block_width], weight_down[index_tp * block_width:(index_tp + 1) * block_width], preferred_element_type=jnp.float32)
            running = running + partial_value.astype(jnp.bfloat16).astype(jnp.float32)
        return running.astype(jnp.bfloat16)
    outputs = lax.map(expert_apply, (buffer, gate_serve, up_serve, down_serve))
    picked = outputs[flat_ids.reshape(-1), row_index.reshape(-1)].reshape(TOKENS, TOP, D).astype(jnp.float32)
    shares = route_weights / lax.optimization_barrier(jnp.sum(route_weights, axis=-1, keepdims=True))
    mixed = lax.optimization_barrier(jnp.sum(shares[:, :, None] * picked, axis=1)).astype(jnp.bfloat16)
    return (gate_serve, up_serve, down_serve, mixed)
```

```python
import jax
import jax.numpy as jnp
from jax import lax
from jax.sharding import PartitionSpec as P

epsilon = 1e-06


def on_device(tokens, norm_gain, gate_train, up_train, down_train, expert_ids, route_weights):
    fs_count = lax.axis_size("fs")
    tp_count = lax.axis_size("tp")
    my_tp = lax.axis_index("tp")
    experts, rows_gate, cols_gate = gate_train.shape
    rows_down, cols_down = down_train.shape[1:]
    tok_rows, picks = expert_ids.shape
    width = tokens.shape[1]
    capacity = 2 * tok_rows * picks // experts
    quarter = capacity // tp_count
    bf16, f32 = jnp.bfloat16, jnp.float32

    gate_cast = (norm_gain[None, :, None] * gate_train).astype(bf16)
    up_cast = (norm_gain[None, :, None] * up_train).astype(bf16)
    both = lax.all_to_all(
        jnp.concatenate([gate_cast, up_cast], axis=2), "fs", split_axis=0, concat_axis=0, tiled=True
    ).reshape(1, fs_count * rows_gate, 2 * cols_gate)
    gate_serve, up_serve = both[:, :, :cols_gate], both[:, :, cols_gate:]
    down_rows = lax.all_to_all(
        down_train.astype(bf16), "fs", split_axis=0, concat_axis=0, tiled=True
    ).reshape(tp_count, fs_count * rows_down // tp_count, cols_down)
    down_cols = lax.all_to_all(down_rows, "tp", split_axis=0, concat_axis=0, tiled=True)
    down_serve = jnp.swapaxes(down_cols, 0, 1).reshape(1, down_rows.shape[1], width)
    gate_whole, up_whole, down_whole = (
        lax.all_gather(gate_serve[0], "tp", axis=1, tiled=True),
        lax.all_gather(up_serve[0], "tp", axis=1, tiled=True),
        lax.all_gather(down_serve[0], "tp", axis=0, tiled=True),
    )

    tok_float = tokens.astype(f32)
    normed = (
        tok_float * lax.rsqrt(jnp.mean(tok_float * tok_float, axis=-1, keepdims=True) + epsilon)
    ).astype(bf16)
    lane = jnp.arange(experts, dtype=jnp.int32)[None, :]
    hot = [expert_ids[:, k][:, None] == lane for k in range(picks)]
    named = sum(h.astype(bf16) for h in hot)
    at = jnp.arange(tok_rows, dtype=jnp.int32)
    before = jnp.dot((at[None, :] < at[:, None]).astype(bf16), named, preferred_element_type=f32)
    slot = [jnp.sum(jnp.where(h, before, 0.0), axis=1).astype(jnp.int32) for h in hot]
    target = [expert_ids[:, k] * capacity + slot[k] for k in range(picks)]

    mine = jnp.arange(experts * quarter, dtype=jnp.int32)
    mine = (mine // quarter) * capacity + my_tp * quarter + mine % quarter
    dispatch = sum((mine[:, None] == t[None, :]).astype(bf16) for t in target)
    outgoing = jnp.dot(dispatch, normed, preferred_element_type=f32).astype(bf16)
    routed = lax.all_to_all(
        outgoing.reshape(experts, quarter, width), "fs", split_axis=0, concat_axis=0, tiled=True
    ).reshape(fs_count * quarter, width)

    gate_act = jnp.dot(routed, gate_whole, preferred_element_type=f32)
    up_act = jnp.dot(routed, up_whole, preferred_element_type=f32)
    hidden = (jax.nn.silu(gate_act) * up_act).astype(bf16)
    results = jnp.dot(hidden, down_whole, preferred_element_type=f32).astype(bf16)
    results = results.reshape(fs_count, quarter, tp_count, width // tp_count)
    results = jnp.swapaxes(results, 1, 2).reshape(fs_count * tp_count, quarter, width // tp_count)
    returned = lax.all_to_all(results, ("fs", "tp"), split_axis=0, concat_axis=0, tiled=True)
    returned = returned.reshape(experts * capacity, width // tp_count)

    slot_ids = jnp.arange(experts * capacity, dtype=jnp.int32)
    total = jnp.sum(route_weights, axis=-1)
    mixed = 0.0
    for k in range(picks):
        selector = (target[k][:, None] == slot_ids[None, :]).astype(bf16)
        picked = jnp.dot(selector, returned, preferred_element_type=f32)
        mixed = mixed + (route_weights[:, k] / total)[:, None] * picked
    return (gate_serve, up_serve, down_serve, mixed.astype(bf16))


def solution(mesh):
    return jax.shard_map(
        on_device,
        mesh=mesh,
        in_specs=(
            P("fs", None),
            P("fs"),
            P(None, "fs", "tp"),
            P(None, "fs", "tp"),
            P(None, "fs", "tp"),
            P("fs", None),
            P("fs", None),
        ),
        out_specs=(P("fs", None, "tp"), P("fs", None, "tp"), P("fs", "tp", None), P("fs", "tp")),
        check_vma=False,
    )
```
